256 devices in a mesh: sp: 32 (over z, y), tp: 8 (over x, core).
Axes of the slice: x: 4, y: 4, z: 8, core: 2. Of those that a mesh axis runs over, the one named last changes fastest.
Arguments:
- queries: bfloat16 [9216, 2048], P('sp', 'tp'), as said below
- key_vectors: bfloat16 [9216, 2048], P('sp', 'tp'), as said below
- latents: bfloat16 [9216, 2048], P('sp'), as said below
- value_weight: bfloat16 [2048, 2048], P(None, 'tp'), as said below
- log_sums: float32 [9216, 32], P('sp', 'tp'), as said below
- out_first: bfloat16 [9216, 2048], P('sp', 'tp'), as said below
- out_second: bfloat16 [9216, 2048], P('sp', 'tp'), as said below
- cotangent: bfloat16 [9216, 2048], P('sp', 'tp'), may hold values from -6 to 6
- head_lambda: float32 [16], P('tp'), may hold values from 0.3 to 0.8
Outputs:
- grad_queries: float32 [9216, 2048], P('sp', 'tp')
- grad_keys: float32 [9216, 2048], P('sp', 'tp')
- grad_latents: bfloat16 [9216, 2048], P('sp', 'tp')
- grad_weight: float32 [2048, 2048], P('sp', 'tp')
The draws below stay inside these ranges and needn't reach their ends.
Inputs may be any that keep to these rules, and one draw needn't show every extreme that they name: queries with entries of standard deviation 1.75. `key_vectors`: keys with entries of standard deviation 1. `latents`: inputs of standard deviation 1. `value_weight`: weights scaled by the inverse square root of 2048. `log_sums`: each row's log-sum of exponentials of its causal scores, for the given queries and keys. `out_first`: the first map's attention output for the given queries, keys, values and log-sums. `out_second`: the second map's attention output, likewise.
All inputs are finite; a program needn't handle non-finite values.
Results may differ from the reference program's by a relative error of at most 0.022.
Values may be sent and summed in bfloat16 or wider, within the bound.
No kernel may reach another device: no remote copies, remote signals or barrier semaphores. Data moves between devices by JAX's collectives and lax.ppermute only.
A program may use at most 192 MiB of HBM per device.

```python
import jax
import jax.numpy as jnp
from jax import lax

D = 2048
HEADS = 16
DH = 64
DV = 128
TOK_DEV = 288
TOKENS = 9216
N_SP = 32
N_TP = 8


def build_inputs(key):
    queries = (1.75 * jax.random.normal(jax.random.fold_in(key, 101), (TOKENS, HEADS * 2 * DH), jnp.float32)).astype(jnp.bfloat16)
    key_vectors = jax.random.normal(jax.random.fold_in(key, 102), (TOKENS, HEADS * 2 * DH), jnp.float32).astype(jnp.bfloat16)
    latents = jax.random.normal(jax.random.fold_in(key, 103), (TOKENS, D), jnp.float32).astype(jnp.bfloat16)
    value_weight = (jax.random.normal(jax.random.fold_in(key, 104), (D, HEADS * DV), jnp.float32) * D ** (-0.5)).astype(jnp.bfloat16)
    values = jnp.dot(latents, value_weight, preferred_element_type=jnp.float32).astype(jnp.bfloat16)
    blocks = TOKENS // TOK_DEV
    query_heads = queries.astype(jnp.float32).reshape(blocks, TOK_DEV, HEADS, 2, DH)
    key_heads = key_vectors.astype(jnp.float32).reshape(TOKENS, HEADS, 2, DH)
    value_heads = values.astype(jnp.float32).reshape(TOKENS, HEADS, DV)
    positions = jnp.arange(TOKENS, dtype=jnp.int32)

    def one_block(pair):
        block_rows, block_index = pair
        query_pos = block_index * TOK_DEV + jnp.arange(TOK_DEV, dtype=jnp.int32)
        scores = jnp.einsum('nhad,mhad->hanm', block_rows, key_heads) * DH ** (-0.5)
        causal = query_pos[:, None] >= positions[None, :]
        scores = jnp.where(causal, scores, -1e+30)
        highest = jnp.max(scores, axis=-1, keepdims=True)
        expo = jnp.exp(scores - highest)
        total = jnp.sum(expo, axis=-1, keepdims=True)
        outputs = jnp.einsum('hanm,mhe->nhae', expo / total, value_heads)
        sums = (highest + jnp.log(total))[..., 0].transpose(2, 0, 1)
        return (sums, outputs)
    sums, outputs = lax.map(one_block, (query_heads, jnp.arange(blocks, dtype=jnp.int32)))
    log_sums = sums.reshape(TOKENS, HEADS * 2)
    out_first = outputs[:, :, :, 0, :].reshape(TOKENS, HEADS * DV).astype(jnp.bfloat16)
    out_second = outputs[:, :, :, 1, :].reshape(TOKENS, HEADS * DV).astype(jnp.bfloat16)
    return (queries, key_vectors, latents, value_weight, log_sums, out_first, out_second)


def draw_queries(key, part):
    return build_inputs(key)[0]


def draw_key_vectors(key, part):
    return build_inputs(key)[1]


def draw_latents(key, part):
    return build_inputs(key)[2]


def draw_value_weight(key, part):
    return build_inputs(key)[3]


def draw_log_sums(key, part):
    return build_inputs(key)[4]


def draw_out_first(key, part):
    return build_inputs(key)[5]


def draw_out_second(key, part):
    return build_inputs(key)[6]


def strengthened(entries, key, source, target, shards_of, factor):
    def block_of(dim):
        return (jnp.arange(entries.shape[dim]) // (entries.shape[dim] // shards_of)).reshape((-1,) + (1,) * (entries.ndim - 1 - dim))

    one_side = jax.random.permutation(key, shards_of)[block_of(target)]
    far = (block_of(target) + shards_of // 2) % shards_of
    return jnp.where((block_of(source) == one_side) | (block_of(source) == far), factor * entries, entries)


def block_scale(key, extent, shards, least, largest):
    factor_of = 1.0
    for dim, blocks in shards:
        steps = jax.random.uniform(jax.random.fold_in(jax.random.fold_in(key, 6), dim), (blocks,), jnp.float32, least / len(shards), largest / len(shards))
        factor_of = factor_of * jnp.repeat(jnp.exp(steps), extent[dim] // blocks).reshape((-1,) + (1,) * (len(extent) - 1 - dim))
    return factor_of


def noise_with(own_key, extent, spread, limit, cuts, heavy, kind=jnp.bfloat16):
    result = spread * jax.random.normal(own_key, extent, jnp.float32)
    if cuts:
        result = result * block_scale(own_key, extent, cuts, -0.22, 0.18)
    return jnp.clip(strengthened(result, jax.random.fold_in(own_key, 3), *heavy), -limit, limit).astype(kind)


def setup_inputs(seed: int = 0) -> dict:
    arg_keys = jax.random.split(jax.random.key(seed), 10)
    return {
        "queries": draw_queries(jax.random.fold_in(arg_keys[9], 71), 0),
        "key_vectors": draw_key_vectors(jax.random.fold_in(arg_keys[9], 71), 0),
        "latents": draw_latents(jax.random.fold_in(arg_keys[9], 71), 0),
        "value_weight": draw_value_weight(jax.random.fold_in(arg_keys[9], 71), 0),
        "log_sums": draw_log_sums(jax.random.fold_in(arg_keys[9], 71), 0),
        "out_first": draw_out_first(jax.random.fold_in(arg_keys[9], 71), 0),
        "out_second": draw_out_second(jax.random.fold_in(arg_keys[9], 71), 0),
        "cotangent": noise_with(arg_keys[7], (TOKENS, HEADS * DV), 1.0, 6.0, ((0, 32), (1, 8)), (0, 1, 32, 2.75)),
        "head_lambda": jnp.clip(0.3 + 0.5 * jax.random.uniform(arg_keys[8], (HEADS,), jnp.float32) ** block_scale(arg_keys[8], (HEADS,), ((0, 8),), -0.2, 0.2), 0.3, 0.8),
    }


def row_terms(out_first, out_second, cotangent, head_lambda):
    count = out_first.shape[0]
    head_count = head_lambda.shape[0]
    first = out_first.astype(jnp.float32).reshape(count, head_count, DV)
    second = out_second.astype(jnp.float32).reshape(count, head_count, DV)
    mixed = first - head_lambda[None, :, None] * second
    inverse = lax.rsqrt(lax.optimization_barrier(jnp.mean(mixed * mixed, axis=-1, keepdims=True)) + 1e-06)
    normed = mixed * inverse
    grad_out = cotangent.astype(jnp.float32).reshape(count, head_count, DV)
    grad_mixed = inverse * (grad_out - normed * lax.optimization_barrier(jnp.mean(grad_out * normed, axis=-1, keepdims=True)))
    grad_rows = grad_mixed.astype(jnp.bfloat16)
    widened = lax.optimization_barrier(grad_rows).astype(jnp.float32)
    row_dots = jnp.stack([lax.optimization_barrier(jnp.sum(widened * first, axis=-1)), lax.optimization_barrier(jnp.sum(widened * second, axis=-1))], axis=-1)
    return (grad_rows.reshape(count, head_count * DV), row_dots.reshape(count, head_count * 2))

def block_grads(query_rows, grad_rows, lse_rows, dot_rows, query_pos, key_rows, value_rows, key_pos, head_lambda):
    count = query_rows.shape[0]
    width = key_rows.shape[0]
    head_count = head_lambda.shape[0]
    score_scale = DH ** (-0.5)
    query_heads = query_rows.astype(jnp.float32).reshape(count, head_count, 2, DH)
    key_heads = key_rows.astype(jnp.float32).reshape(width, head_count, 2, DH)
    grad_heads = grad_rows.astype(jnp.float32).reshape(count, head_count, DV)
    value_heads = value_rows.astype(jnp.float32).reshape(width, head_count, DV)
    scores = jnp.einsum('nhad,mhad->hanm', query_heads, key_heads) * score_scale
    causal = query_pos[:, None] >= key_pos[None, :]
    shifts = lse_rows.reshape(count, head_count, 2).transpose(1, 2, 0)[..., None]
    probs = jnp.exp(jnp.where(causal, scores - shifts, -1e+30))
    d_attn = jnp.einsum('nhe,mhe->hnm', grad_heads, value_heads)
    dots = dot_rows.reshape(count, head_count, 2).transpose(1, 2, 0)[..., None]
    map_weight = jnp.stack([jnp.ones_like(head_lambda), -head_lambda], axis=1)[:, :, None, None]
    d_scores = (map_weight * probs * (d_attn[:, None] - dots)).astype(jnp.bfloat16)
    d_scores = lax.optimization_barrier(d_scores).astype(jnp.float32)
    weights = (probs[:, 0] - head_lambda[:, None, None] * probs[:, 1]).astype(jnp.bfloat16)
    weights = lax.optimization_barrier(weights).astype(jnp.float32)
    grad_q = jnp.einsum('hanm,mhad->nhad', d_scores, key_heads) * score_scale
    grad_k = jnp.einsum('hanm,nhad->mhad', d_scores, query_heads) * score_scale
    grad_v = jnp.einsum('hnm,nhe->mhe', weights, grad_heads)
    return (grad_q.reshape(count, -1), grad_k.reshape(width, -1), grad_v.reshape(width, -1))

def reference(queries, key_vectors, latents, value_weight, log_sums, out_first, out_second, cotangent, head_lambda):
    values = jnp.dot(latents, value_weight, preferred_element_type=jnp.float32).astype(jnp.bfloat16)
    grad_rows, row_dots = row_terms(out_first, out_second, cotangent, head_lambda)
    positions = jnp.arange(TOKENS, dtype=jnp.int32)

    def per_head(index):
        query_head = lax.dynamic_slice_in_dim(queries, index * 2 * DH, 2 * DH, 1)
        key_head = lax.dynamic_slice_in_dim(key_vectors, index * 2 * DH, 2 * DH, 1)
        value_head = lax.dynamic_slice_in_dim(values, index * DV, DV, 1)
        grad_head = lax.dynamic_slice_in_dim(grad_rows, index * DV, DV, 1)
        lse_head = lax.dynamic_slice_in_dim(log_sums, index * 2, 2, 1)
        dot_head = lax.dynamic_slice_in_dim(row_dots, index * 2, 2, 1)
        lambda_one = lax.dynamic_slice_in_dim(head_lambda, index, 1, 0)

        def block_step(totals, block_index):
            first_row = (block_index * TOK_DEV).astype(jnp.int32)
            query_pos = first_row + jnp.arange(TOK_DEV, dtype=jnp.int32)
            grad_q, grad_k, grad_v = block_grads(lax.dynamic_slice_in_dim(query_head, first_row, TOK_DEV, 0), lax.dynamic_slice_in_dim(grad_head, first_row, TOK_DEV, 0), lax.dynamic_slice_in_dim(lse_head, first_row, TOK_DEV, 0), lax.dynamic_slice_in_dim(dot_head, first_row, TOK_DEV, 0), query_pos, key_head, value_head, positions, lambda_one)
            return ((totals[0] + grad_k, totals[1] + grad_v), grad_q)
        initial = (jnp.zeros((TOKENS, 2 * DH), jnp.float32), jnp.zeros((TOKENS, DV), jnp.float32))
        totals, grad_blocks = lax.scan(block_step, initial, jnp.arange(N_SP, dtype=jnp.int32))
        return (grad_blocks.reshape(TOKENS, 2 * DH), totals[0], totals[1])
    grad_q, grad_k, grad_v = lax.map(per_head, jnp.arange(HEADS, dtype=jnp.int32))
    grad_queries = grad_q.transpose(1, 0, 2).reshape(TOKENS, HEADS * 2 * DH)
    grad_keys = grad_k.transpose(1, 0, 2).reshape(TOKENS, HEADS * 2 * DH)
    grad_values = grad_v.transpose(1, 0, 2).reshape(TOKENS, HEADS * DV).astype(jnp.bfloat16)
    grad_weight = lax.dot_general(latents, grad_values, (((0,), (0,)), ((), ())), preferred_element_type=jnp.float32)
    value_groups = grad_values.reshape(TOKENS, N_TP, -1).transpose(1, 0, 2)
    weight_groups = value_weight.reshape(D, N_TP, -1).transpose(1, 0, 2)

    def add_group(total, pair):
        partial_sum = lax.dot_general(pair[0], pair[1], (((1,), (1,)), ((), ())), preferred_element_type=jnp.float32)
        rounded = lax.optimization_barrier(partial_sum.astype(jnp.bfloat16))
        return (total + rounded.astype(jnp.float32), None)
    latent_total, unused = lax.scan(add_group, jnp.zeros((TOKENS, D), jnp.float32), (value_groups, weight_groups))
    return (grad_queries, grad_keys, latent_total.astype(jnp.bfloat16), grad_weight)
```

```python
import functools

import jax
import jax.numpy as jnp
from jax import lax
from jax.experimental import pallas as pl
from jax.experimental.pallas import tpu as pltpu
from jax.sharding import PartitionSpec as P


DH = 64
DV = 128
NZ = 8
NY = 4
STAT_ROWS = 16
GROUPS = [(0,), (1, 7), (2, 6), (3, 5), (4,)]
VMEM_LIMIT = 24 * 2**20
F32 = jnp.float32
BF16 = jnp.bfloat16
NN = (((1,), (0,)), ((), ()))
NT = (((1,), (1,)), ((), ()))
TN = (((0,), (0,)), ((), ()))


def dot(a, b, dims=NN):
    return lax.dot_general(a, b, dims, preferred_element_type=F32)


def pack_rows_kernel(lam_ref, q_ref, first_ref, second_ref, cot_ref, lse_ref, out_ref):
    n = q_ref.shape[0]
    out_ref[0:n, 0 : 2 * DV] = q_ref[...]
    piece_row = lax.broadcasted_iota(jnp.int32, (STAT_ROWS, DV), 0)
    stats = lse_ref[...]
    for h in range(2):
        cols = slice(h * DV, (h + 1) * DV)
        lam = lam_ref[h]
        first = first_ref[:, cols].astype(F32)
        second = second_ref[:, cols].astype(F32)
        mixed = first - lam * second
        inverse = lax.rsqrt(jnp.mean(mixed * mixed, axis=-1, keepdims=True) + 1e-06)
        normed = mixed * inverse
        grad_out = cot_ref[:, cols].astype(F32)
        grad_mixed = inverse * (grad_out - normed * jnp.mean(grad_out * normed, axis=-1, keepdims=True))
        grad_rows = grad_mixed.astype(BF16)
        out_ref[0:n, 2 * DV + h * DV : 2 * DV + (h + 1) * DV] = grad_rows
        widened = grad_rows.astype(F32)
        for m, side in enumerate((first, second)):
            product = widened * side
            high = product.astype(BF16)
            low = (product - high.astype(F32)).astype(BF16)
            row = 8 + 2 * h + m
            pick = jnp.where((piece_row == row) | (piece_row == row + 4), 1.0, 0.0).astype(BF16)
            stats = stats + dot(pick, high, NT) + dot(pick, low, NT)
    high = stats.astype(BF16).astype(F32)
    is_low = (lax.broadcasted_iota(jnp.int32, stats.shape, 0) & 4) != 0
    out_ref[n : n + STAT_ROWS, :] = jnp.zeros((STAT_ROWS, 4 * DV), BF16)
    out_ref[n : n + STAT_ROWS, 0:n] = jnp.where(is_low, stats - high, high).astype(BF16)


def pack_keys_kernel(key_ref, latent_ref, weight_ref, out_ref):
    out_ref[:, 0 : 2 * DV] = key_ref[...]
    out_ref[:, 2 * DV :] = dot(latent_ref[...], weight_ref[...]).astype(BF16)


def attention_kernel(offsets, first_call, last_call, zy_ref, lam_ref, *refs):
    count = len(offsets)
    row_refs, refs = refs[:count], refs[count:]
    kv_ref, refs = refs[0], refs[1:]
    if not first_call:
        acc_in, refs = refs[0], refs[1:]
    dq_refs, refs = refs[:count], refs[count:]
    if last_call:
        total_refs, (acc_ref, kz_ref) = refs[: 2 * NY], refs[2 * NY :]
    else:
        acc_ref, kz_ref = refs
    width = kv_ref.shape[0]
    n = width // NY
    z = zy_ref[0]
    y = zy_ref[1]
    tile = 384 if width % 384 == 0 else 128

    low_lanes = lax.broadcasted_iota(jnp.int32, (1, DV), 1) < DH
    for h in range(2):
        k = kv_ref[:, h * DV : (h + 1) * DV]
        kz_ref[2 * h] = jnp.where(low_lanes, k, jnp.zeros_like(k))
        kz_ref[2 * h + 1] = jnp.where(low_lanes, jnp.zeros_like(k), k)
    if first_call:
        acc_ref[...] = jnp.zeros_like(acc_ref)
    else:
        acc_ref[...] = acc_in[...]

    def cell(rows_ref, dq_ref, diagonal):
        def head(h, carry):
            cols = pl.ds(pl.multiple_of(h * DV, DV), DV)
            grad_cols = pl.ds(pl.multiple_of((h + 2) * DV, DV), DV)
            lam = lam_ref[h]
            q = rows_ref[0:n, cols] * jnp.asarray(DH ** (-0.5), BF16)
            zeros = jnp.zeros_like(q)
            q0 = jnp.where(low_lanes, q, zeros)
            q1 = jnp.where(low_lanes, zeros, q)
            g = rows_ref[0:n, grad_cols]
            stats = rows_ref[n : n + STAT_ROWS, 0:n]
            piece_row = lax.broadcasted_iota(jnp.int32, (STAT_ROWS, DV), 0)

            def stat(row):
                pick = jnp.where((piece_row == row) | (piece_row == row + 4), 1.0, 0.0)
                return jnp.concatenate([dot(stats, pick.astype(BF16), TN)] * (tile // DV), axis=1)

            lse0, lse1 = stat(2 * h), stat(2 * h + 1)
            dot0, dot1 = stat(2 * h + 8), stat(2 * h + 9)
            dq = jnp.zeros((n, DV), F32)
            both_q = jnp.concatenate([q0, q1], axis=0)
            for t in range(width // tile):
                span = slice(t * tile, (t + 1) * tile)
                k = kv_ref[span, cols]
                v = kv_ref[span, grad_cols]
                s0 = dot(q0, k, NT) - lse0
                s1 = dot(q1, k, NT) - lse1
                if diagonal:
                    key = lax.broadcasted_iota(jnp.int32, (1, tile), 1) + t * tile
                    block = (key >= n).astype(jnp.int32) + (key >= 2 * n).astype(jnp.int32) + (key >= 3 * n).astype(jnp.int32)
                    bound = jnp.where(block == 0, key, jnp.where(y + block >= NY, -1, n))
                    seen = lax.broadcasted_iota(jnp.int32, (n, tile), 0) >= bound
                    s0 = jnp.where(seen, s0, -1e30)
                    s1 = jnp.where(seen, s1, -1e30)
                p0 = jnp.exp(s0)
                p1 = lam * jnp.exp(s1)
                d_attn = dot(g, v, NT)
                ds0 = (p0 * (d_attn - dot0)).astype(BF16)
                ds1 = (p1 * (dot1 - d_attn)).astype(BF16)
                weights = (p0 - p1).astype(BF16)
                dq = dq + dot(ds0, kz_ref[2 * h, span, :]) + dot(ds1, kz_ref[2 * h + 1, span, :])
                both_ds = jnp.concatenate([ds0, ds1], axis=0)
                acc_ref[cols, span] += dot(both_q, both_ds, TN)
                acc_ref[grad_cols, span] += dot(g, weights, TN)
            dq_ref[:, cols] = dq.astype(dq_ref.dtype)
            return carry

        lax.fori_loop(0, 2, head, 0)

    for rows_ref, dq_ref, offset in zip(row_refs, dq_refs, offsets):
        if offset == 0:
            cell(rows_ref, dq_ref, True)
        else:
            pl.when(z + offset < NZ)(functools.partial(cell, rows_ref, dq_ref, False))
    if last_call:
        for t in range(width // DV):
            turned = acc_ref[:, t * DV : (t + 1) * DV].T.astype(BF16)
            start = t * DV
            while start < (t + 1) * DV:
                e = start // n
                stop = min((t + 1) * DV, (e + 1) * n)
                part = turned[start - t * DV : stop - t * DV]
                total_refs[e][start - e * n : stop - e * n, :] = part[:, 2 * DV :]
                total_refs[NY + e][start - e * n : stop - e * n, :] = part[:, : 2 * DV]
                start = stop


def weight_term_kernel(latent_ref, *refs):
    *part_refs, grad_ref, out_ref = refs
    total = part_refs[0][...].astype(F32)
    for part in part_refs[1:]:
        total = total + part[...].astype(F32)
    grads = total.astype(BF16)
    grad_ref[...] = grads
    out_ref[...] = dot(latent_ref[...], grads, TN).astype(BF16)


def latent_term_kernel(side_ref, grad_ref, weight_ref, kept_ref, sent_ref):
    grads = grad_ref[...]
    count, _, columns = kept_ref.shape
    for out_ref, side in ((kept_ref, side_ref[1]), (sent_ref, 1 - side_ref[1])):
        for j in range(count):
            rows = pl.ds(pl.multiple_of((2 * j + side) * columns, columns), columns)
            out_ref[j] = dot(grads, weight_ref[rows, :], NT).astype(BF16)


def latent_pair_kernel(side_ref, kept_ref, arrived_ref, *out_refs):
    count = kept_ref.shape[0]
    for d, out_ref in enumerate(out_refs):
        j = lax.rem(side_ref[0] + d, count)
        out_ref[...] = (kept_ref[j].astype(F32) + arrived_ref[j].astype(F32)).astype(out_ref.dtype)


def vmem(count):
    return [pl.BlockSpec(memory_space=pltpu.VMEM)] * count


def attention(offsets, first_call, last_call, zy, head_lambda, rows, keys_values, acc):
    n = keys_values.shape[0] // NY
    width = keys_values.shape[0]
    count = len(offsets)
    operands = [zy, head_lambda, *rows, keys_values] + ([] if first_call else [acc])
    total = [jax.ShapeDtypeStruct((4 * DV, width), F32)]
    if last_call:
        total = [jax.ShapeDtypeStruct((n, 2 * DV), BF16)] * (2 * NY)
    scratch = [pltpu.VMEM((4, width, DV), BF16)]
    if last_call:
        scratch = [pltpu.VMEM((4 * DV, width), F32)] + scratch
    smem = [pl.BlockSpec(memory_space=pltpu.SMEM)] * 2
    return pl.pallas_call(
        functools.partial(attention_kernel, offsets, first_call, last_call),
        out_shape=[jax.ShapeDtypeStruct((n, 2 * DV), F32 if d == 0 else BF16) for d in offsets] + total,
        in_specs=smem + vmem(len(operands) - 2),
        out_specs=vmem(count + len(total)),
        scratch_shapes=scratch,
        cost_estimate=pl.CostEstimate(flops=count * 4 * 10**9, bytes_accessed=count * 10**6, transcendentals=0),
        compiler_params=pltpu.CompilerParams(vmem_limit_bytes=VMEM_LIMIT),
    )(*operands)


def ring(size, step):
    return [(i, (i + step) % size) for i in range(size)]


def program(
    queries, key_vectors, latents, value_weight, log_sums, out_first, out_second, cotangent, head_lambda
):
    n = queries.shape[0]
    z = lax.axis_index("z")
    y = lax.axis_index("y")
    zy = jnp.stack([z, y]).astype(jnp.int32)
    sums = log_sums.T
    sums = jnp.concatenate([sums, sums, jnp.zeros((8, n), F32)], axis=0)
    rows = pl.pallas_call(
        pack_rows_kernel,
        out_shape=jax.ShapeDtypeStruct((n + STAT_ROWS, 4 * DV), BF16),
        in_specs=[pl.BlockSpec(memory_space=pltpu.SMEM)] + vmem(5),
        out_specs=vmem(1)[0],
        cost_estimate=pl.CostEstimate(flops=10**9, bytes_accessed=10**6, transcendentals=0),
    )(head_lambda, queries, out_first, out_second, cotangent, sums)
    keys_values = pl.pallas_call(
        pack_keys_kernel,
        out_shape=jax.ShapeDtypeStruct((n, 4 * DV), BF16),
        in_specs=vmem(3),
        out_specs=vmem(1)[0],
        cost_estimate=pl.CostEstimate(flops=10**9, bytes_accessed=3 * 10**6, transcendentals=0),
    )(key_vectors, latents, value_weight)

    blocks = [keys_values] + [lax.ppermute(keys_values, "y", ring(NY, -e)) for e in (1, 2, 3)]
    all_keys = jnp.concatenate(blocks, axis=0)
    ahead = [rows]
    behind = [rows]
    for _ in range(3):
        ahead.append(lax.ppermute(ahead[-1], "z", ring(NZ, -1)))
        behind.append(lax.ppermute(behind[-1], "z", ring(NZ, 1)))
    ahead.append(lax.ppermute(ahead[-1], "z", ring(NZ, -1)))

    source = {d: ahead[d] for d in range(5)} | {8 - d: behind[d] for d in (1, 2, 3)}
    acc = None
    returned = []
    own = None
    for index, offsets in enumerate(GROUPS):
        first, last = index == 0, index == len(GROUPS) - 1
        out = attention(offsets, first, last, zy, head_lambda, [source[d] for d in offsets], all_keys, acc)
        terms, acc = out[: len(offsets)], out[len(offsets) :]
        for d, term in zip(offsets, terms):
            if d == 0:
                own = term
            else:
                returned.append(lax.ppermute(term, "z", [(i, i + d) for i in range(NZ - d)]))
        if not last:
            acc = acc[0]
    value_parts, key_parts = acc[:NY], acc[NY:]
    value_parts = [value_parts[0]] + [lax.ppermute(value_parts[e], "y", ring(NY, e)) for e in (1, 2, 3)]
    key_parts = [key_parts[0]] + [lax.ppermute(key_parts[e], "y", ring(NY, e)) for e in (1, 2, 3)]

    rows_of_weight = latents.shape[1]
    call = pl.pallas_call(
        weight_term_kernel,
        out_shape=[
            jax.ShapeDtypeStruct((n, 2 * DV), BF16),
            jax.ShapeDtypeStruct((rows_of_weight, 2 * DV), BF16),
        ],
        in_specs=vmem(1 + NY),
        out_specs=vmem(2),
        cost_estimate=pl.CostEstimate(flops=10**9, bytes_accessed=3 * 10**6, transcendentals=0),
        compiler_params=pltpu.CompilerParams(vmem_limit_bytes=VMEM_LIMIT),
        name="weight_term",
    )
    values_grad, weight_term = call(latents, *value_parts)
    arrived_weight = lax.all_to_all(
        weight_term.reshape(NZ * NY, -1, 2 * DV), ("z", "y"), split_axis=0, concat_axis=0, tiled=True
    )
    size = lax.axis_size("tp")
    place = lax.axis_index("tp")
    side = jnp.stack([place // 2, place % 2]).astype(jnp.int32)
    columns = rows_of_weight // size
    smem = [pl.BlockSpec(memory_space=pltpu.SMEM)]
    kept, sent = pl.pallas_call(
        latent_term_kernel,
        out_shape=[jax.ShapeDtypeStruct((size // 2, n, columns), BF16)] * 2,
        in_specs=smem + vmem(2),
        out_specs=vmem(2),
        cost_estimate=pl.CostEstimate(flops=10**9, bytes_accessed=3 * 10**6, transcendentals=0),
        compiler_params=pltpu.CompilerParams(vmem_limit_bytes=VMEM_LIMIT),
        name="latent_term",
    )(side, values_grad, value_weight)
    arrived = lax.ppermute(sent, "tp", [(i, i ^ 1) for i in range(size)])
    latent_parts = pl.pallas_call(
        latent_pair_kernel,
        out_shape=[jax.ShapeDtypeStruct((n, columns), F32 if d == 0 else BF16) for d in range(size // 2)],
        in_specs=smem + vmem(2),
        out_specs=vmem(size // 2),
        cost_estimate=pl.CostEstimate(flops=10**8, bytes_accessed=10**6, transcendentals=0),
        compiler_params=pltpu.CompilerParams(vmem_limit_bytes=VMEM_LIMIT),
        name="latent_pair",
    )(side, kept, arrived)
    grad_latents = latent_parts[0]
    for d in range(1, size // 2):
        grad_latents = grad_latents + lax.ppermute(latent_parts[d], "tp", ring(size, 2 * d)).astype(F32)
    grad_latents = grad_latents.astype(BF16)

    grad_queries = own
    for term in returned:
        grad_queries = grad_queries + term.astype(F32)
    grad_queries = grad_queries * DH ** (-0.5)
    grad_keys = key_parts[0].astype(F32)
    for part in key_parts[1:]:
        grad_keys = grad_keys + part.astype(F32)
    grad_weight = arrived_weight.astype(F32).sum(axis=0)
    return (grad_queries, grad_keys, grad_latents, grad_weight)


def solution(mesh):
    devices = mesh.devices
    grid = jax.sharding.Mesh(devices.reshape(NZ, NY, devices.shape[1]), ("z", "y", "tp"))
    rows = ("z", "y")
    return jax.shard_map(
        program,
        mesh=grid,
        in_specs=(
            P(rows, "tp"),
            P(rows, "tp"),
            P(rows, None),
            P(None, "tp"),
            P(rows, "tp"),
            P(rows, "tp"),
            P(rows, "tp"),
            P(rows, "tp"),
            P("tp"),
        ),
        out_specs=(P(rows, "tp"), P(rows, "tp"), P(rows, "tp"), P(rows, "tp")),
        check_vma=False,
    )
```

```python
import functools

import jax
import jax.numpy as jnp
from jax import lax
from jax.experimental import pallas as pl
from jax.experimental.pallas import tpu as pltpu
from jax.sharding import PartitionSpec as P


DH = 64
DV = 128
NZ = 8
NY = 4
STAT_ROWS = 16
GROUPS = [(0,), (1, 7), (2, 6), (3, 4, 5)]
VMEM_LIMIT = 24 * 2**20
F32 = jnp.float32
BF16 = jnp.bfloat16
NN = (((1,), (0,)), ((), ()))
NT = (((1,), (1,)), ((), ()))
TN = (((0,), (0,)), ((), ()))


def dot(a, b, dims=NN):
    return lax.dot_general(a, b, dims, preferred_element_type=F32)


def pack_rows_kernel(lam_ref, q_ref, first_ref, second_ref, cot_ref, lse_ref, out_ref):
    n = q_ref.shape[0]
    out_ref[0:n, 0 : 2 * DV] = q_ref[...]
    piece_row = lax.broadcasted_iota(jnp.int32, (STAT_ROWS, DV), 0)
    stats = lse_ref[...]
    for h in range(2):
        cols = slice(h * DV, (h + 1) * DV)
        lam = lam_ref[h]
        first = first_ref[:, cols].astype(F32)
        second = second_ref[:, cols].astype(F32)
        mixed = first - lam * second
        inverse = lax.rsqrt(jnp.mean(mixed * mixed, axis=-1, keepdims=True) + 1e-06)
        normed = mixed * inverse
        grad_out = cot_ref[:, cols].astype(F32)
        grad_mixed = inverse * (grad_out - normed * jnp.mean(grad_out * normed, axis=-1, keepdims=True))
        grad_rows = grad_mixed.astype(BF16)
        out_ref[0:n, 2 * DV + h * DV : 2 * DV + (h + 1) * DV] = grad_rows
        widened = grad_rows.astype(F32)
        for m, side in enumerate((first, second)):
            product = widened * side
            high = product.astype(BF16)
            low = (product - high.astype(F32)).astype(BF16)
            row = 8 + 2 * h + m
            pick = jnp.where((piece_row == row) | (piece_row == row + 4), 1.0, 0.0).astype(BF16)
            stats = stats + dot(pick, high, NT) + dot(pick, low, NT)
    high = stats.astype(BF16).astype(F32)
    is_low = (lax.broadcasted_iota(jnp.int32, stats.shape, 0) & 4) != 0
    out_ref[n : n + STAT_ROWS, :] = jnp.zeros((STAT_ROWS, 4 * DV), BF16)
    out_ref[n : n + STAT_ROWS, 0:n] = jnp.where(is_low, stats - high, high).astype(BF16)


def pack_keys_kernel(key_ref, latent_ref, weight_ref, out_ref):
    out_ref[:, 0 : 2 * DV] = key_ref[...]
    out_ref[:, 2 * DV :] = dot(latent_ref[...], weight_ref[...]).astype(BF16)


def attention_kernel(offsets, first_call, last_call, zy_ref, lam_ref, *refs):
    count = len(offsets)
    row_refs, refs = refs[:count], refs[count:]
    kv_ref, refs = refs[0], refs[1:]
    if not first_call:
        acc_in, refs = refs[0], refs[1:]
    dq_refs, refs = refs[:count], refs[count:]
    if count > 2:
        *refs, all_rows_ref, all_dq_ref = refs
    if last_call:
        total_refs, (acc_ref, kz_ref) = refs[: 2 * NY], refs[2 * NY :]
    else:
        acc_ref, kz_ref = refs
    width = kv_ref.shape[0]
    n = width // NY
    z = zy_ref[0]
    y = zy_ref[1]
    tiles = [width // 256 * 128, width - width // 256 * 128]
    starts = [0, tiles[0]]

    low_lanes = lax.broadcasted_iota(jnp.int32, (1, DV), 1) < DH
    for h in range(2):
        k = kv_ref[:, h * DV : (h + 1) * DV]
        kz_ref[2 * h] = jnp.where(low_lanes, k, jnp.zeros_like(k))
        kz_ref[2 * h + 1] = jnp.where(low_lanes, jnp.zeros_like(k), k)
    if first_call:
        acc_ref[...] = jnp.zeros_like(acc_ref)
    else:
        acc_ref[...] = acc_in[...]

    def cells(rows_of, dq_of, live, diagonal):
        def head(step, carry):
            h = step % 2
            rows_ref, dq_ref = rows_of(step // 2), dq_of(step // 2)
            cols = pl.ds(pl.multiple_of(h * DV, DV), DV)
            grad_cols = pl.ds(pl.multiple_of((h + 2) * DV, DV), DV)
            lam = lam_ref[h]
            q = rows_ref[0:n, cols] * jnp.asarray(DH ** (-0.5), BF16)
            zeros = jnp.zeros_like(q)
            q0 = jnp.where(low_lanes, q, zeros)
            q1 = jnp.where(low_lanes, zeros, q)
            g = rows_ref[0:n, grad_cols]
            stats = rows_ref[n : n + STAT_ROWS, 0:n]
            piece_row = lax.broadcasted_iota(jnp.int32, (STAT_ROWS, DV), 0)

            def stat(row):
                pick = jnp.where((piece_row == row) | (piece_row == row + 4), 1.0, 0.0)
                return dot(stats, pick.astype(BF16), TN)

            lse0, lse1 = stat(2 * h), stat(2 * h + 1)
            dot0, dot1 = stat(2 * h + 8), stat(2 * h + 9)
            dq = jnp.zeros((n, DV), F32)
            both_q = jnp.concatenate([q0, q1], axis=0)
            for start, tile in zip(starts, tiles):
                span = slice(start, start + tile)

                def wide(x):
                    return jnp.concatenate([x] * (tile // DV), axis=1)

                k = kv_ref[span, cols]
                v = kv_ref[span, grad_cols]
                s0 = dot(q0, k, NT) - wide(lse0)
                s1 = dot(q1, k, NT) - wide(lse1)
                if diagonal:
                    key = lax.broadcasted_iota(jnp.int32, (1, tile), 1) + start
                    block = (key >= n).astype(jnp.int32) + (key >= 2 * n).astype(jnp.int32) + (key >= 3 * n).astype(jnp.int32)
                    bound = jnp.where(block == 0, key, jnp.where(y + block >= NY, -1, n))
                    seen = lax.broadcasted_iota(jnp.int32, (n, tile), 0) >= bound
                    s0 = jnp.where(seen, s0, -1e30)
                    s1 = jnp.where(seen, s1, -1e30)
                p0 = jnp.exp(s0)
                p1 = lam * jnp.exp(s1)
                d_attn = dot(g, v, NT)
                ds0 = (p0 * (d_attn - wide(dot0))).astype(BF16)
                ds1 = (p1 * (wide(dot1) - d_attn)).astype(BF16)
                weights = (p0 - p1).astype(BF16)
                dq = dq + dot(ds0, kz_ref[2 * h, span, :]) + dot(ds1, kz_ref[2 * h + 1, span, :])
                both_ds = jnp.concatenate([ds0, ds1], axis=0)
                acc_ref[cols, span] += dot(both_q, both_ds, TN)
                acc_ref[grad_cols, span] += dot(g, weights, TN)
            dq_ref[:, cols] = dq.astype(dq_ref.dtype)
            return carry

        lax.fori_loop(0, 2 * live, head, 0)

    live = [(z + offset < NZ).astype(jnp.int32) for offset in offsets]
    if count < 3:
        for i, offset in enumerate(offsets):
            cells(lambda _, i=i: row_refs[i], lambda _, i=i: dq_refs[i], live[i], offset == 0)
    else:
        for i, rows_ref in enumerate(row_refs):
            all_rows_ref[i] = rows_ref[...]
        cells(all_rows_ref.at.__getitem__, all_dq_ref.at.__getitem__, sum(live), False)
        for i, dq_ref in enumerate(dq_refs):
            dq_ref[...] = all_dq_ref[i]
    if last_call:
        for t in range(width // DV):
            turned = acc_ref[:, t * DV : (t + 1) * DV].T.astype(BF16)
            start = t * DV
            while start < (t + 1) * DV:
                e = start // n
                stop = min((t + 1) * DV, (e + 1) * n)
                part = turned[start - t * DV : stop - t * DV]
                total_refs[e][start - e * n : stop - e * n, :] = part[:, 2 * DV :]
                total_refs[NY + e][start - e * n : stop - e * n, :] = part[:, : 2 * DV]
                start = stop


def sum_kernel(scale, *refs):
    *part_refs, out_ref = refs
    total = part_refs[0][...].astype(F32)
    for part in part_refs[1:]:
        total = total + part[...].astype(F32)
    if scale != 1.0:
        total = total * scale
    out_ref[...] = total.astype(out_ref.dtype)


def weight_term_kernel(latent_ref, *refs):
    *part_refs, grad_ref, out_ref = refs
    total = part_refs[0][...].astype(F32)
    for part in part_refs[1:]:
        total = total + part[...].astype(F32)
    grads = total.astype(BF16)
    grad_ref[...] = grads
    out_ref[...] = dot(latent_ref[...], grads, TN).astype(BF16)


def latent_term_kernel(side_ref, grad_ref, weight_ref, kept_ref, sent_ref):
    grads = grad_ref[...]
    count, _, columns = kept_ref.shape
    for out_ref, side in ((kept_ref, side_ref[1]), (sent_ref, 1 - side_ref[1])):
        for j in range(count):
            rows = pl.ds(pl.multiple_of((2 * j + side) * columns, columns), columns)
            out_ref[j] = dot(grads, weight_ref[rows, :], NT).astype(BF16)


def latent_pair_kernel(side_ref, kept_ref, arrived_ref, *out_refs):
    count = kept_ref.shape[0]
    for d, out_ref in enumerate(out_refs):
        j = lax.rem(side_ref[0] + d, count)
        out_ref[...] = (kept_ref[j].astype(F32) + arrived_ref[j].astype(F32)).astype(out_ref.dtype)


def vmem(count):
    return [pl.BlockSpec(memory_space=pltpu.VMEM)] * count


def attention(offsets, first_call, last_call, zy, head_lambda, rows, keys_values, acc):
    n = keys_values.shape[0] // NY
    width = keys_values.shape[0]
    count = len(offsets)
    operands = [zy, head_lambda, *rows, keys_values] + ([] if first_call else [acc])
    total = [jax.ShapeDtypeStruct((4 * DV, width), F32)]
    if last_call:
        total = [jax.ShapeDtypeStruct((n, 2 * DV), BF16)] * (2 * NY)
    scratch = [pltpu.VMEM((4, width, DV), BF16)]
    if last_call:
        scratch = [pltpu.VMEM((4 * DV, width), F32)] + scratch
    if count > 2:
        scratch += [pltpu.VMEM((count, n + STAT_ROWS, 4 * DV), BF16), pltpu.VMEM((count, n, 2 * DV), BF16)]
    smem = [pl.BlockSpec(memory_space=pltpu.SMEM)] * 2
    return pl.pallas_call(
        functools.partial(attention_kernel, offsets, first_call, last_call),
        out_shape=[jax.ShapeDtypeStruct((n, 2 * DV), F32 if d == 0 else BF16) for d in offsets] + total,
        in_specs=smem + vmem(len(operands) - 2),
        out_specs=vmem(count + len(total)),
        scratch_shapes=scratch,
        cost_estimate=pl.CostEstimate(flops=count * 4 * 10**9, bytes_accessed=count * 10**6, transcendentals=0),
        compiler_params=pltpu.CompilerParams(vmem_limit_bytes=VMEM_LIMIT),
    )(*operands)


def gather_kernel(parts_ref, out_ref):
    total = parts_ref[0].astype(F32)
    for i in range(1, parts_ref.shape[0]):
        total = total + parts_ref[i].astype(F32)
    out_ref[...] = total


def added(parts, dtype, scale=1.0):
    return pl.pallas_call(
        functools.partial(sum_kernel, scale),
        out_shape=jax.ShapeDtypeStruct(parts[0].shape, dtype),
        in_specs=vmem(len(parts)),
        out_specs=vmem(1)[0],
        cost_estimate=pl.CostEstimate(flops=10**8, bytes_accessed=10**6, transcendentals=0),
        compiler_params=pltpu.CompilerParams(vmem_limit_bytes=VMEM_LIMIT),
        name="added",
    )(*parts)


def ring(size, step):
    return [(i, (i + step) % size) for i in range(size)]


def program(
    queries, key_vectors, latents, value_weight, log_sums, out_first, out_second, cotangent, head_lambda
):
    n = queries.shape[0]
    z = lax.axis_index("z")
    y = lax.axis_index("y")
    zy = jnp.stack([z, y]).astype(jnp.int32)
    sums = log_sums.T
    sums = jnp.concatenate([sums, sums, jnp.zeros((8, n), F32)], axis=0)
    rows = pl.pallas_call(
        pack_rows_kernel,
        out_shape=jax.ShapeDtypeStruct((n + STAT_ROWS, 4 * DV), BF16),
        in_specs=[pl.BlockSpec(memory_space=pltpu.SMEM)] + vmem(5),
        out_specs=vmem(1)[0],
        cost_estimate=pl.CostEstimate(flops=10**9, bytes_accessed=10**6, transcendentals=0),
    )(head_lambda, queries, out_first, out_second, cotangent, sums)
    keys_values = pl.pallas_call(
        pack_keys_kernel,
        out_shape=jax.ShapeDtypeStruct((n, 4 * DV), BF16),
        in_specs=vmem(3),
        out_specs=vmem(1)[0],
        cost_estimate=pl.CostEstimate(flops=10**9, bytes_accessed=3 * 10**6, transcendentals=0),
    )(key_vectors, latents, value_weight)

    half = n // 2
    after = lax.ppermute(keys_values, "y", ring(NY, -1))
    before = lax.ppermute(keys_values, "y", ring(NY, 1))
    upper = lax.ppermute(after[:half], "y", ring(NY, -1))
    lower = lax.ppermute(before[half:], "y", ring(NY, 1))
    all_keys = jnp.concatenate([keys_values, after, upper, lower, before], axis=0)
    ahead = [rows]
    behind = [rows]
    for t in range(1, 5):
        ahead.append(lax.ppermute(ahead[-1], "z", [(k + 1, k) for k in range(NZ - t)]))
        if t < 4:
            behind.append(lax.ppermute(behind[-1], "z", [((k + t + 4) % NZ, (k + t + 5) % NZ) for k in range(3)]))
    smem = [pl.BlockSpec(memory_space=pltpu.SMEM)]
    source = {d: ahead[d] for d in range(5)} | {8 - d: behind[d] for d in (1, 2, 3)}
    acc = None
    returned = []
    parts = {}
    own = None
    for index, offsets in enumerate(GROUPS):
        first, last = index == 0, index == len(GROUPS) - 1
        out = attention(offsets, first, last, zy, head_lambda, [source[d] for d in offsets], all_keys, acc)
        terms, acc = out[: len(offsets)], out[len(offsets) :]
        for d, term in zip(offsets, terms):
            if d == 0:
                own = term
            else:
                parts[d] = term
                if d < 3 or d > 4:
                    returned.append(lax.ppermute(term, "z", [(i, i + d) for i in range(NZ - d)]))
        if not last:
            acc = acc[0]
    value_parts, key_parts = acc[:NY], acc[NY:]
    hop = lax.ppermute(parts[4], "z", [(i, i + 1) for i in range(NZ - 4)])
    joined = added([parts[3], hop], BF16)
    returned.append(lax.ppermute(joined, "z", [(i, i + 3) for i in range(NZ - 3)]))
    value_parts = [value_parts[0]] + [lax.ppermute(value_parts[e], "y", ring(NY, e)) for e in (1, 2, 3)]
    key_parts = [key_parts[0]] + [lax.ppermute(key_parts[e], "y", ring(NY, e)) for e in (1, 2, 3)]

    rows_of_weight = latents.shape[1]
    call = pl.pallas_call(
        weight_term_kernel,
        out_shape=[
            jax.ShapeDtypeStruct((n, 2 * DV), BF16),
            jax.ShapeDtypeStruct((rows_of_weight, 2 * DV), BF16),
        ],
        in_specs=vmem(1 + NY),
        out_specs=vmem(2),
        cost_estimate=pl.CostEstimate(flops=10**9, bytes_accessed=3 * 10**6, transcendentals=0),
        compiler_params=pltpu.CompilerParams(vmem_limit_bytes=VMEM_LIMIT),
        name="weight_term",
    )
    values_grad, weight_term = call(latents, *value_parts)
    arrived_weight = lax.all_to_all(
        weight_term.reshape(NZ * NY, -1, 2 * DV), ("z", "y"), split_axis=0, concat_axis=0, tiled=True
    )
    size = lax.axis_size("tp")
    place = lax.axis_index("tp")
    side = jnp.stack([place // 2, place % 2]).astype(jnp.int32)
    columns = rows_of_weight // size
    kept, sent = pl.pallas_call(
        latent_term_kernel,
        out_shape=[jax.ShapeDtypeStruct((size // 2, n, columns), BF16)] * 2,
        in_specs=smem + vmem(2),
        out_specs=vmem(2),
        cost_estimate=pl.CostEstimate(flops=10**9, bytes_accessed=3 * 10**6, transcendentals=0),
        compiler_params=pltpu.CompilerParams(vmem_limit_bytes=VMEM_LIMIT),
        name="latent_term",
    )(side, values_grad, value_weight)
    arrived = lax.ppermute(sent, "tp", [(i, i ^ 1) for i in range(size)])
    call = pl.pallas_call(
        latent_pair_kernel,
        out_shape=[jax.ShapeDtypeStruct((n, columns), F32 if d == 0 else BF16) for d in range(size // 2)],
        in_specs=smem + vmem(2),
        out_specs=vmem(size // 2),
        cost_estimate=pl.CostEstimate(flops=10**8, bytes_accessed=10**6, transcendentals=0),
        compiler_params=pltpu.CompilerParams(vmem_limit_bytes=VMEM_LIMIT),
        name="latent_pair",
    )
    latent_parts = call(side, kept, arrived)
    grad_latents = latent_parts[0]
    for d in range(1, size // 2):
        grad_latents = grad_latents + lax.ppermute(latent_parts[d], "tp", ring(size, 2 * d)).astype(F32)
    grad_latents = grad_latents.astype(BF16)

    grad_queries = added([own, *returned], F32, DH ** (-0.5))
    grad_keys = added(key_parts, F32)
    grad_weight = pl.pallas_call(
        gather_kernel,
        out_shape=jax.ShapeDtypeStruct(arrived_weight.shape[1:], F32),
        in_specs=vmem(1),
        out_specs=vmem(1)[0],
        cost_estimate=pl.CostEstimate(flops=10**8, bytes_accessed=10**6, transcendentals=0),
        compiler_params=pltpu.CompilerParams(vmem_limit_bytes=VMEM_LIMIT),
        name="weight_sum",
    )(arrived_weight)
    return (grad_queries, grad_keys, grad_latents, grad_weight)


def solution(mesh):
    devices = mesh.devices
    grid = jax.sharding.Mesh(devices.reshape(NZ, NY, devices.shape[1]), ("z", "y", "tp"))
    rows = ("z", "y")
    return jax.shard_map(
        program,
        mesh=grid,
        in_specs=(
            P(rows, "tp"),
            P(rows, "tp"),
            P(rows, None),
            P(None, "tp"),
            P(rows, "tp"),
            P(rows, "tp"),
            P(rows, "tp"),
            P(rows, "tp"),
            P("tp"),
        ),
        out_specs=(P(rows, "tp"), P(rows, "tp"), P(rows, "tp"), P(rows, "tp")),
        check_vma=False,
    )
```

```python
import functools

import jax
import jax.numpy as jnp
from jax import lax
from jax.experimental import pallas as pl
from jax.experimental.pallas import tpu as pltpu
from jax.sharding import PartitionSpec as P


DH = 64
DV = 128
NZ = 8
NY = 4
STAT_ROWS = 16
GROUPS = [(0,), (1, 7), (2, 6), (3, 4, 5)]
VMEM_LIMIT = 24 * 2**20
F32 = jnp.float32
BF16 = jnp.bfloat16
NN = (((1,), (0,)), ((), ()))
NT = (((1,), (1,)), ((), ()))
TN = (((0,), (0,)), ((), ()))


def dot(a, b, dims=NN):
    return lax.dot_general(a, b, dims, preferred_element_type=F32)


def pack_rows_kernel(lam_ref, q_ref, first_ref, second_ref, cot_ref, lse_ref, out_ref):
    n = q_ref.shape[0]
    out_ref[0:n, 0 : 2 * DV] = q_ref[...]
    piece_row = lax.broadcasted_iota(jnp.int32, (STAT_ROWS, DV), 0)
    stats = lse_ref[...]
    for h in range(2):
        cols = slice(h * DV, (h + 1) * DV)
        lam = lam_ref[h]
        first = first_ref[:, cols].astype(F32)
        second = second_ref[:, cols].astype(F32)
        mixed = first - lam * second
        inverse = lax.rsqrt(jnp.mean(mixed * mixed, axis=-1, keepdims=True) + 1e-06)
        normed = mixed * inverse
        grad_out = cot_ref[:, cols].astype(F32)
        grad_mixed = inverse * (grad_out - normed * jnp.mean(grad_out * normed, axis=-1, keepdims=True))
        grad_rows = grad_mixed.astype(BF16)
        out_ref[0:n, 2 * DV + h * DV : 2 * DV + (h + 1) * DV] = grad_rows
        widened = grad_rows.astype(F32)
        for m, side in enumerate((first, second)):
            product = widened * side
            high = product.astype(BF16)
            low = (product - high.astype(F32)).astype(BF16)
            row = 8 + 2 * h + m
            pick = jnp.where((piece_row == row) | (piece_row == row + 4), 1.0, 0.0).astype(BF16)
            stats = stats + dot(pick, high, NT) + dot(pick, low, NT)
    high = stats.astype(BF16).astype(F32)
    is_low = (lax.broadcasted_iota(jnp.int32, stats.shape, 0) & 4) != 0
    out_ref[n : n + STAT_ROWS, :] = jnp.zeros((STAT_ROWS, 4 * DV), BF16)
    out_ref[n : n + STAT_ROWS, 0:n] = jnp.where(is_low, stats - high, high).astype(BF16)


def pack_keys_kernel(key_ref, latent_ref, weight_ref, out_ref, total_ref):
    step = pl.program_id(0)
    term = dot(latent_ref[...], weight_ref[...])

    @pl.when(step == 0)
    def _():
        out_ref[:, 0 : 2 * DV] = key_ref[...]
        total_ref[...] = term

    @pl.when(step > 0)
    def _():
        total_ref[...] += term

    @pl.when(step == pl.num_programs(0) - 1)
    def _():
        out_ref[:, 2 * DV :] = total_ref[...].astype(BF16)


def attention_kernel(offsets, first_call, last_call, zy_ref, lam_ref, *refs):
    count = len(offsets)
    row_refs, refs = refs[:count], refs[count:]
    kv_ref, refs = refs[0], refs[1:]
    if not first_call:
        acc_in, refs = refs[0], refs[1:]
    dq_refs, refs = refs[:count], refs[count:]
    if count > 2:
        *refs, all_rows_ref, all_dq_ref = refs
    if last_call:
        total_refs, (acc_ref, kz_ref) = refs[: 2 * NY], refs[2 * NY :]
    else:
        acc_ref, kz_ref = refs
    width = kv_ref.shape[0]
    n = width // NY
    z = zy_ref[0]
    y = zy_ref[1]
    tiles = [width // 256 * 128, width - width // 256 * 128]
    starts = [0, tiles[0]]

    low_lanes = lax.broadcasted_iota(jnp.int32, (1, DV), 1) < DH
    for h in range(2):
        k = kv_ref[:, h * DV : (h + 1) * DV]
        kz_ref[2 * h] = jnp.where(low_lanes, k, jnp.zeros_like(k))
        kz_ref[2 * h + 1] = jnp.where(low_lanes, jnp.zeros_like(k), k)
    if first_call:
        acc_ref[...] = jnp.zeros_like(acc_ref)
    else:
        acc_ref[...] = acc_in[...]

    def cells(rows_of, dq_of, live, diagonal):
        def head(step, carry):
            h = step % 2
            rows_ref, dq_ref = rows_of(step // 2), dq_of(step // 2)
            cols = pl.ds(pl.multiple_of(h * DV, DV), DV)
            grad_cols = pl.ds(pl.multiple_of((h + 2) * DV, DV), DV)
            lam = lam_ref[h]
            q = rows_ref[0:n, cols] * jnp.asarray(DH ** (-0.5), BF16)
            zeros = jnp.zeros_like(q)
            q0 = jnp.where(low_lanes, q, zeros)
            q1 = jnp.where(low_lanes, zeros, q)
            g = rows_ref[0:n, grad_cols]
            stats = rows_ref[n : n + STAT_ROWS, 0:n]
            piece_row = lax.broadcasted_iota(jnp.int32, (STAT_ROWS, DV), 0)

            def stat(row):
                pick = jnp.where((piece_row == row) | (piece_row == row + 4), 1.0, 0.0)
                return dot(stats, pick.astype(BF16), TN)

            lse0, lse1 = stat(2 * h), stat(2 * h + 1)
            dot0, dot1 = stat(2 * h + 8), stat(2 * h + 9)
            dq = jnp.zeros((n, DV), F32)
            both_q = jnp.concatenate([q0, q1], axis=0)
            for start, tile in zip(starts, tiles):
                span = slice(start, start + tile)

                def wide(x):
                    return jnp.concatenate([x] * (tile // DV), axis=1)

                k = kv_ref[span, cols]
                v = kv_ref[span, grad_cols]
                s0 = dot(q0, k, NT) - wide(lse0)
                s1 = dot(q1, k, NT) - wide(lse1)
                if diagonal:
                    key = lax.broadcasted_iota(jnp.int32, (1, tile), 1) + start
                    block = (key >= n).astype(jnp.int32) + (key >= 2 * n).astype(jnp.int32) + (key >= 3 * n).astype(jnp.int32)
                    bound = jnp.where(block == 0, key, jnp.where(y + block >= NY, -1, n))
                    seen = lax.broadcasted_iota(jnp.int32, (n, tile), 0) >= bound
                    s0 = jnp.where(seen, s0, -1e30)
                    s1 = jnp.where(seen, s1, -1e30)
                p0 = jnp.exp(s0)
                p1 = lam * jnp.exp(s1)
                d_attn = dot(g, v, NT)
                ds0 = (p0 * (d_attn - wide(dot0))).astype(BF16)
                ds1 = (p1 * (wide(dot1) - d_attn)).astype(BF16)
                weights = (p0 - p1).astype(BF16)
                dq = dq + dot(ds0, kz_ref[2 * h, span, :]) + dot(ds1, kz_ref[2 * h + 1, span, :])
                both_ds = jnp.concatenate([ds0, ds1], axis=0)
                acc_ref[cols, span] += dot(both_q, both_ds, TN)
                acc_ref[grad_cols, span] += dot(g, weights, TN)
            dq_ref[:, cols] = dq.astype(dq_ref.dtype)
            return carry

        lax.fori_loop(0, 2 * live, head, 0)

    live = [(z + offset < NZ).astype(jnp.int32) for offset in offsets]
    if count < 3:
        for i, offset in enumerate(offsets):
            cells(lambda _, i=i: row_refs[i], lambda _, i=i: dq_refs[i], live[i], offset == 0)
    else:
        for i, rows_ref in enumerate(row_refs):
            all_rows_ref[i] = rows_ref[...]
        cells(all_rows_ref.at.__getitem__, all_dq_ref.at.__getitem__, sum(live), False)
        for i, dq_ref in enumerate(dq_refs):
            dq_ref[...] = all_dq_ref[i]
    if last_call:
        for t in range(width // DV):
            turned = acc_ref[:, t * DV : (t + 1) * DV].T.astype(BF16)
            start = t * DV
            while start < (t + 1) * DV:
                e = start // n
                stop = min((t + 1) * DV, (e + 1) * n)
                part = turned[start - t * DV : stop - t * DV]
                total_refs[e][start - e * n : stop - e * n, :] = part[:, 2 * DV :]
                total_refs[NY + e][start - e * n : stop - e * n, :] = part[:, : 2 * DV]
                start = stop


def sum_kernel(scale, *refs):
    *part_refs, out_ref = refs
    total = part_refs[0][...].astype(F32)
    for part in part_refs[1:]:
        total = total + part[...].astype(F32)
    if scale != 1.0:
        total = total * scale
    out_ref[...] = total.astype(out_ref.dtype)


def weight_term_kernel(latent_ref, *refs):
    *part_refs, grad_ref, out_ref = refs
    total = part_refs[0][...].astype(F32)
    for part in part_refs[1:]:
        total = total + part[...].astype(F32)
    grads = total.astype(BF16)
    grad_ref[...] = grads
    out_ref[...] = dot(latent_ref[...], grads, TN).astype(BF16)


def latent_term_kernel(side_ref, grad_ref, weight_ref, kept_ref, sent_ref):
    grads = grad_ref[...]
    count, _, columns = kept_ref.shape
    for out_ref, side in ((kept_ref, side_ref[1]), (sent_ref, 1 - side_ref[1])):
        for j in range(count):
            rows = pl.ds(pl.multiple_of((2 * j + side) * columns, columns), columns)
            out_ref[j] = dot(grads, weight_ref[rows, :], NT).astype(BF16)


def latent_pair_kernel(side_ref, kept_ref, arrived_ref, *out_refs):
    count = kept_ref.shape[0]
    for d, out_ref in enumerate(out_refs):
        j = lax.rem(side_ref[0] + d, count)
        out_ref[...] = (kept_ref[j].astype(F32) + arrived_ref[j].astype(F32)).astype(out_ref.dtype)


def vmem(count):
    return [pl.BlockSpec(memory_space=pltpu.VMEM)] * count


def attention(offsets, first_call, last_call, zy, head_lambda, rows, keys_values, acc):
    n = keys_values.shape[0] // NY
    width = keys_values.shape[0]
    count = len(offsets)
    operands = [zy, head_lambda, *rows, keys_values] + ([] if first_call else [acc])
    total = [jax.ShapeDtypeStruct((4 * DV, width), F32)]
    if last_call:
        total = [jax.ShapeDtypeStruct((n, 2 * DV), BF16)] * (2 * NY)
    scratch = [pltpu.VMEM((4, width, DV), BF16)]
    if last_call:
        scratch = [pltpu.VMEM((4 * DV, width), F32)] + scratch
    if count > 2:
        scratch += [pltpu.VMEM((count, n + STAT_ROWS, 4 * DV), BF16), pltpu.VMEM((count, n, 2 * DV), BF16)]
    smem = [pl.BlockSpec(memory_space=pltpu.SMEM)] * 2
    return pl.pallas_call(
        functools.partial(attention_kernel, offsets, first_call, last_call),
        out_shape=[jax.ShapeDtypeStruct((n, 2 * DV), F32 if d == 0 else BF16) for d in offsets] + total,
        in_specs=smem + vmem(len(operands) - 2),
        out_specs=vmem(count + len(total)),
        scratch_shapes=scratch,
        cost_estimate=pl.CostEstimate(flops=count * 4 * 10**9, bytes_accessed=count * 10**6, transcendentals=0),
        compiler_params=pltpu.CompilerParams(vmem_limit_bytes=VMEM_LIMIT),
    )(*operands)


def gather_kernel(parts_ref, out_ref):
    total = parts_ref[0].astype(F32)
    for i in range(1, parts_ref.shape[0]):
        total = total + parts_ref[i].astype(F32)
    out_ref[...] = total


def added(parts, dtype, scale=1.0):
    return pl.pallas_call(
        functools.partial(sum_kernel, scale),
        out_shape=jax.ShapeDtypeStruct(parts[0].shape, dtype),
        in_specs=vmem(len(parts)),
        out_specs=vmem(1)[0],
        cost_estimate=pl.CostEstimate(flops=10**8, bytes_accessed=10**6, transcendentals=0),
        compiler_params=pltpu.CompilerParams(vmem_limit_bytes=VMEM_LIMIT),
        name="added",
    )(*parts)


def ring(size, step):
    return [(i, (i + step) % size) for i in range(size)]


def program(
    queries, key_vectors, latents, value_weight, log_sums, out_first, out_second, cotangent, head_lambda
):
    n = queries.shape[0]
    z = lax.axis_index("z")
    y = lax.axis_index("y")
    zy = jnp.stack([z, y]).astype(jnp.int32)
    sums = log_sums.T
    sums = jnp.concatenate([sums, sums, jnp.zeros((8, n), F32)], axis=0)
    rows = pl.pallas_call(
        pack_rows_kernel,
        out_shape=jax.ShapeDtypeStruct((n + STAT_ROWS, 4 * DV), BF16),
        in_specs=[pl.BlockSpec(memory_space=pltpu.SMEM)] + vmem(5),
        out_specs=vmem(1)[0],
        cost_estimate=pl.CostEstimate(flops=10**9, bytes_accessed=10**6, transcendentals=0),
    )(head_lambda, queries, out_first, out_second, cotangent, sums)
    keys_values = pl.pallas_call(
        pack_keys_kernel,
        grid=(4,),
        out_shape=jax.ShapeDtypeStruct((n, 4 * DV), BF16),
        in_specs=[
            pl.BlockSpec((n, 2 * DV), lambda i: (0, 0)),
            pl.BlockSpec((n, latents.shape[1] // 4), lambda i: (0, i)),
            pl.BlockSpec((latents.shape[1] // 4, 2 * DV), lambda i: (i, 0)),
        ],
        out_specs=pl.BlockSpec((n, 4 * DV), lambda i: (0, 0)),
        scratch_shapes=[pltpu.VMEM((n, 2 * DV), F32)],
        cost_estimate=pl.CostEstimate(flops=10**9, bytes_accessed=3 * 10**6, transcendentals=0),
    )(key_vectors, latents, value_weight)

    half = n // 2
    after = lax.ppermute(keys_values, "y", ring(NY, -1))
    before = lax.ppermute(keys_values, "y", ring(NY, 1))
    upper = lax.ppermute(after[:half], "y", ring(NY, -1))
    lower = lax.ppermute(before[half:], "y", ring(NY, 1))
    all_keys = jnp.concatenate([keys_values, after, upper, lower, before], axis=0)
    ahead = [rows]
    behind = [rows]
    for t in range(1, 5):
        ahead.append(lax.ppermute(ahead[-1], "z", [(k + 1, k) for k in range(NZ - t)]))
        if t < 4:
            behind.append(lax.ppermute(behind[-1], "z", [((k + t + 4) % NZ, (k + t + 5) % NZ) for k in range(3)]))
    smem = [pl.BlockSpec(memory_space=pltpu.SMEM)]
    source = {d: ahead[d] for d in range(5)} | {8 - d: behind[d] for d in (1, 2, 3)}
    acc = None
    returned = []
    parts = {}
    own = None
    for index, offsets in enumerate(GROUPS):
        first, last = index == 0, index == len(GROUPS) - 1
        out = attention(offsets, first, last, zy, head_lambda, [source[d] for d in offsets], all_keys, acc)
        terms, acc = out[: len(offsets)], out[len(offsets) :]
        for d, term in zip(offsets, terms):
            if d == 0:
                own = term
            else:
                parts[d] = term
                if d < 3 or d > 4:
                    returned.append(lax.ppermute(term, "z", [(i, i + d) for i in range(NZ - d)]))
        if not last:
            acc = acc[0]
    value_parts, key_parts = acc[:NY], acc[NY:]
    hop = lax.ppermute(parts[4], "z", [(i, i + 1) for i in range(NZ - 4)])
    joined = added([parts[3], hop], BF16)
    returned.append(lax.ppermute(joined, "z", [(i, i + 3) for i in range(NZ - 3)]))
    value_parts = [value_parts[0]] + [lax.ppermute(value_parts[e], "y", ring(NY, e)) for e in (1, 2, 3)]
    key_parts = [key_parts[0]] + [lax.ppermute(key_parts[e], "y", ring(NY, e)) for e in (1, 2, 3)]

    rows_of_weight = latents.shape[1]
    call = pl.pallas_call(
        weight_term_kernel,
        out_shape=[
            jax.ShapeDtypeStruct((n, 2 * DV), BF16),
            jax.ShapeDtypeStruct((rows_of_weight, 2 * DV), BF16),
        ],
        in_specs=vmem(1 + NY),
        out_specs=vmem(2),
        cost_estimate=pl.CostEstimate(flops=10**9, bytes_accessed=3 * 10**6, transcendentals=0),
        compiler_params=pltpu.CompilerParams(vmem_limit_bytes=VMEM_LIMIT),
        name="weight_term",
    )
    values_grad, weight_term = call(latents, *value_parts)
    arrived_weight = lax.all_to_all(
        weight_term.reshape(NZ * NY, -1, 2 * DV), ("z", "y"), split_axis=0, concat_axis=0, tiled=True
    )
    size = lax.axis_size("tp")
    place = lax.axis_index("tp")
    side = jnp.stack([place // 2, place % 2]).astype(jnp.int32)
    columns = rows_of_weight // size
    kept, sent = pl.pallas_call(
        latent_term_kernel,
        out_shape=[jax.ShapeDtypeStruct((size // 2, n, columns), BF16)] * 2,
        in_specs=smem + vmem(2),
        out_specs=vmem(2),
        cost_estimate=pl.CostEstimate(flops=10**9, bytes_accessed=3 * 10**6, transcendentals=0),
        compiler_params=pltpu.CompilerParams(vmem_limit_bytes=VMEM_LIMIT),
        name="latent_term",
    )(side, values_grad, value_weight)
    arrived = lax.ppermute(sent, "tp", [(i, i ^ 1) for i in range(size)])
    call = pl.pallas_call(
        latent_pair_kernel,
        out_shape=[jax.ShapeDtypeStruct((n, columns), F32 if d == 0 else BF16) for d in range(size // 2)],
        in_specs=smem + vmem(2),
        out_specs=vmem(size // 2),
        cost_estimate=pl.CostEstimate(flops=10**8, bytes_accessed=10**6, transcendentals=0),
        compiler_params=pltpu.CompilerParams(vmem_limit_bytes=VMEM_LIMIT),
        name="latent_pair",
    )
    latent_parts = call(side, kept, arrived)
    grad_latents = latent_parts[0]
    for d in range(1, size // 2):
        grad_latents = grad_latents + lax.ppermute(latent_parts[d], "tp", ring(size, 2 * d)).astype(F32)
    grad_latents = grad_latents.astype(BF16)

    grad_queries = added([own, *returned], F32, DH ** (-0.5))
    grad_keys = added(key_parts, F32)
    grad_weight = pl.pallas_call(
        gather_kernel,
        out_shape=jax.ShapeDtypeStruct(arrived_weight.shape[1:], F32),
        in_specs=vmem(1),
        out_specs=vmem(1)[0],
        cost_estimate=pl.CostEstimate(flops=10**8, bytes_accessed=10**6, transcendentals=0),
        compiler_params=pltpu.CompilerParams(vmem_limit_bytes=VMEM_LIMIT),
        name="weight_sum",
    )(arrived_weight)
    return (grad_queries, grad_keys, grad_latents, grad_weight)


def solution(mesh):
    devices = mesh.devices
    grid = jax.sharding.Mesh(devices.reshape(NZ, NY, devices.shape[1]), ("z", "y", "tp"))
    rows = ("z", "y")
    return jax.shard_map(
        program,
        mesh=grid,
        in_specs=(
            P(rows, "tp"),
            P(rows, "tp"),
            P(rows, None),
            P(None, "tp"),
            P(rows, "tp"),
            P(rows, "tp"),
            P(rows, "tp"),
            P(rows, "tp"),
            P("tp"),
        ),
        out_specs=(P(rows, "tp"), P(rows, "tp"), P(rows, "tp"), P(rows, "tp")),
        check_vma=False,
    )
```
